256 devices in a mesh: sp: 64 (over z, y, core), tp: 4 (over x).
Axes of the slice: x: 4, y: 4, z: 8, core: 2. Of those that a mesh axis runs over, the one named last changes fastest.
Arguments:
- resid: bfloat16 [12288, 2048], P(('sp', 'tp')), may hold values from -6 to 6
- query_a: bfloat16 [12288, 1024], P('sp', 'tp'), may hold values from -12 to 12
- key_a: bfloat16 [12288, 1024], P('sp', 'tp'), may hold values from -12 to 12
- value_a: bfloat16 [12288, 1024], P('sp', 'tp'), may hold values from -6 to 6
- query_b: bfloat16 [12288, 128], P('sp', 'tp'), may hold values from -12 to 12
- key_b: bfloat16 [12288, 128], P('sp', 'tp'), may hold values from -12 to 12
- value_b: bfloat16 [12288, 128], P('sp', 'tp'), may hold values from -6 to 6
- out_a: bfloat16 [1024, 2048], P('tp'), may hold values from -0.1875 to 0.1875
- out_b: bfloat16 [128, 2048], P('tp'), may hold values from -0.5 to 0.5
- attn_gain: float32 [2048], replicated, may hold values from 0.1 to 1.9
- mlp_gain: float32 [2048], replicated, may hold values from 0.1 to 1.9
- gate_weight: bfloat16 [2048, 5632], P('sp', 'tp'), may hold values from -0.125 to 0.125
- up_weight: bfloat16 [2048, 5632], P('sp', 'tp'), may hold values from -0.125 to 0.125
- down_weight: bfloat16 [5632, 2048], P('tp', 'sp'), may hold values from -0.078125 to 0.078125
Outputs:
- result: bfloat16 [12288, 2048], P(('sp', 'tp'))
The draws below stay inside these ranges and needn't reach their ends.
All inputs are finite; a program needn't handle non-finite values.
Results may differ from the reference program's by a relative error of at most 0.014.
Values may be sent and summed in bfloat16 or wider, within the bound.
A program may use at most 128 MiB of HBM per device.

```python
import math
import jax
import jax.numpy as jnp
from jax import lax

D = 2048
HEADS_A = 4
HEAD_A = 256
HEADS_B = 4
HEAD_B = 32
FF = 5632
TOKENS = 12288
N_TP = 4


def paired(key, salt, heads, size):
    base = jax.random.fold_in(key, salt)
    parts = jax.random.split(base, 5)
    direction = jax.random.normal(parts[0], (heads, size), jnp.float32)
    direction = direction / jnp.sqrt(jnp.sum(direction * direction, axis=-1, keepdims=True))
    order = jax.random.permutation(parts[1], heads)
    fast_count = heads // 2
    fast = order < fast_count
    levels = jnp.where(fast, math.log(1.0 / 40.0) - 0.5, math.log(1.5 / TOKENS) - 0.5)
    drift = jax.random.uniform(parts[4], (TOKENS // 32, heads), jnp.float32, -0.7, 0.7)
    drift = jnp.repeat(drift, 32, axis=0)
    rough_query = jnp.clip(jax.random.normal(parts[2], (TOKENS, heads, size), jnp.float32), -4.0, 4.0)
    rough_key = jnp.clip(jax.random.normal(parts[3], (TOKENS, heads, size), jnp.float32), -4.0, 4.0)
    rough_key = rough_key - jnp.sum(rough_key * direction, axis=-1, keepdims=True) * direction
    query = rough_query + math.sqrt(size) * direction
    keyed = rough_key + (levels[None, :] + drift)[:, :, None] * direction
    query = jnp.clip(query, -12.0, 12.0).reshape(TOKENS, heads * size)
    keyed = jnp.clip(keyed, -12.0, 12.0).reshape(TOKENS, heads * size)
    return (query, keyed)


def draw_query_a(key, part):
    return paired(key, 11, HEADS_A, HEAD_A)[0].astype(jnp.bfloat16)


def draw_key_a(key, part):
    return paired(key, 11, HEADS_A, HEAD_A)[1].astype(jnp.bfloat16)


def draw_query_b(key, part):
    return paired(key, 12, HEADS_B, HEAD_B)[0].astype(jnp.bfloat16)


def draw_key_b(key, part):
    return paired(key, 12, HEADS_B, HEAD_B)[1].astype(jnp.bfloat16)


def shard_levels(key, shape, cuts, smallest, top_value):
    level, own = 1.0, jax.random.fold_in(key, 6)
    for position, blocks in cuts:
        draws = jnp.exp(jax.random.uniform(jax.random.fold_in(own, position), (blocks,), jnp.float32, smallest / len(cuts), top_value / len(cuts)))
        level = level * jnp.repeat(draws, shape[position] // blocks).reshape([-1 if axis == position else 1 for axis in range(len(shape))])
    return level


def gaussian(stream_key, dims, spread, reach, cuts=(), held_as=jnp.bfloat16):
    values = jax.random.normal(stream_key, dims, jnp.float32) * spread
    if len(cuts) > 0:
        values = shard_levels(stream_key, dims, cuts, -0.22, 0.18) * values
    return jnp.clip(values, min=-reach, max=reach).astype(held_as)


def setup_inputs(seed: int = 0) -> dict:
    arg_keys = jax.random.split(jax.random.key(seed), 15)
    return {
        "resid": gaussian(arg_keys[0], (TOKENS, D), 1.0, 6.0, ((0, 256),)),
        "query_a": draw_query_a(jax.random.fold_in(arg_keys[14], 71), 0),
        "key_a": draw_key_a(jax.random.fold_in(arg_keys[14], 71), 0),
        "value_a": gaussian(arg_keys[3], (TOKENS, HEADS_A * HEAD_A), 1.0, 6.0, ((0, 64), (1, 4))),
        "query_b": draw_query_b(jax.random.fold_in(arg_keys[14], 71), 0),
        "key_b": draw_key_b(jax.random.fold_in(arg_keys[14], 71), 0),
        "value_b": gaussian(arg_keys[6], (TOKENS, HEADS_B * HEAD_B), 1.0, 6.0, ((0, 64), (1, 4))),
        "out_a": gaussian(arg_keys[7], (HEADS_A * HEAD_A, D), (HEADS_A * HEAD_A) ** -0.5, 0.1875, ((0, 4),)),
        "out_b": gaussian(arg_keys[8], (HEADS_B * HEAD_B, D), (HEADS_B * HEAD_B) ** -0.5, 0.5, ((0, 4),)),
        "attn_gain": jnp.clip(1.0 + 0.18 * jax.random.normal(arg_keys[9], (D,), jnp.float32), 0.1, 1.9),
        "mlp_gain": jnp.clip(1.0 + 0.18 * jax.random.normal(arg_keys[10], (D,), jnp.float32), 0.1, 1.9),
        "gate_weight": gaussian(arg_keys[11], (D, FF), D ** -0.5, 0.125, ((0, 64), (1, 4))),
        "up_weight": gaussian(arg_keys[12], (D, FF), D ** -0.5, 0.125, ((0, 64), (1, 4))),
        "down_weight": gaussian(arg_keys[13], (FF, D), FF ** -0.5, 0.078125, ((0, 4), (1, 64))),
    }


epsilon = 1e-06

def stick_weights(queries, key_rows, anchor, factor):
    amount = queries.shape[0]
    heads = queries.shape[1]
    length = key_rows.shape[0]
    block_len = min(512, length)
    sub_len = min(128, block_len)
    block_count = length // block_len
    sub_count = block_len // sub_len
    key_tiles = key_rows.reshape(block_count, block_len, heads, key_rows.shape[2])
    inner_mask = (jnp.arange(sub_len)[:, None] > jnp.arange(sub_len)[None, :]).astype(jnp.float32)
    outer_mask = (jnp.arange(sub_count)[:, None] > jnp.arange(sub_count)[None, :]).astype(jnp.float32)
    query_pos = anchor + jnp.arange(amount, dtype=jnp.int32)

    def step(suffix, inputs):
        key_tile, block_id = inputs
        scores = jnp.einsum('qhd,khd->qhk', queries.astype(jnp.float32), key_tile.astype(jnp.float32)) * factor
        key_pos = block_id * block_len + jnp.arange(block_len, dtype=jnp.int32)
        causal = (key_pos[None, :] < query_pos[:, None])[:, None, :]
        log_keep = jnp.where(causal, jax.nn.log_sigmoid(-scores), 0.0)
        split_keep = log_keep.reshape(amount, heads, sub_count, sub_len)
        within = jnp.einsum('qhcj,js->qhcs', split_keep, inner_mask, precision=lax.Precision.HIGHEST)
        sub_totals = lax.optimization_barrier(jnp.sum(split_keep, axis=-1))
        after_sub = jnp.einsum('qhc,cd->qhd', sub_totals, outer_mask, precision=lax.Precision.HIGHEST)
        later_sum = (within + after_sub[..., None]).reshape(amount, heads, block_len) + suffix[:, :, None]
        log_weight = jnp.where(causal, scores + log_keep + later_sum, -1e+30)
        weight = jnp.exp(log_weight).astype(jnp.bfloat16)
        return (suffix + lax.optimization_barrier(jnp.sum(sub_totals, axis=-1)), weight)
    start_sum = jnp.zeros((amount, heads), jnp.float32)
    ignored, stacked = lax.scan(step, start_sum, (key_tiles, jnp.arange(block_count, dtype=jnp.int32)), reverse=True)
    return jnp.moveaxis(stacked, 0, 2).reshape(amount, heads, length)

def stick_attention(query, keyed, valued, heads, size):
    length = query.shape[0]
    query_heads = query.reshape(length, heads, size)
    key_heads = keyed.reshape(length, heads, size)
    value_heads = valued.reshape(length, heads, size).astype(jnp.float32)
    query_len = min(512, length)

    def one_block(member):
        anchor = (member * query_len).astype(jnp.int32)
        queries = lax.dynamic_slice_in_dim(query_heads, anchor, query_len, 0)
        weights = stick_weights(queries, key_heads, anchor, size ** (-0.5))
        outcome = jnp.einsum('qhk,khd->qhd', weights.astype(jnp.float32), value_heads)
        return outcome.astype(jnp.bfloat16)
    outcome = lax.map(one_block, jnp.arange(length // query_len, dtype=jnp.int32))
    return outcome.reshape(length, heads * size)

def round_trip(values):
    return lax.optimization_barrier(values.astype(jnp.bfloat16)).astype(jnp.float32)

def reference(resid, query_a, key_a, value_a, query_b, key_b, value_b, out_a, out_b, attn_gain, mlp_gain, gate_weight, up_weight, down_weight):
    attended_a = stick_attention(query_a, key_a, value_a, HEADS_A, HEAD_A)
    attended_b = stick_attention(query_b, key_b, value_b, HEADS_B, HEAD_B)
    width_a = HEADS_A * HEAD_A // N_TP
    width_b = HEADS_B * HEAD_B // N_TP
    projected = jnp.zeros((TOKENS, D), jnp.float32)
    for member in range(N_TP):
        cols_a = slice(member * width_a, (member + 1) * width_a)
        cols_b = slice(member * width_b, (member + 1) * width_b)
        piece_sum = jnp.dot(attended_a[:, cols_a], out_a[cols_a], preferred_element_type=jnp.float32)
        piece_sum = piece_sum + jnp.dot(attended_b[:, cols_b], out_b[cols_b], preferred_element_type=jnp.float32)
        projected = projected + round_trip(piece_sum)
    normed = projected * lax.rsqrt(lax.optimization_barrier(jnp.mean(projected * projected, axis=-1, keepdims=True)) + epsilon) * attn_gain.astype(jnp.float32)
    middle = (resid.astype(jnp.float32) + normed).astype(jnp.bfloat16)
    middle_f = middle.astype(jnp.float32)
    channel_input = (middle_f * lax.rsqrt(lax.optimization_barrier(jnp.mean(middle_f * middle_f, axis=-1, keepdims=True)) + epsilon) * mlp_gain.astype(jnp.float32)).astype(jnp.bfloat16)
    hidden_width = FF // N_TP
    mixer_sum = jnp.zeros((TOKENS, D), jnp.float32)
    for member in range(N_TP):
        cols = slice(member * hidden_width, (member + 1) * hidden_width)
        gate_sums = jnp.dot(channel_input, gate_weight[:, cols], preferred_element_type=jnp.float32)
        up_sums = jnp.dot(channel_input, up_weight[:, cols], preferred_element_type=jnp.float32)
        hidden = (jax.nn.silu(gate_sums) * up_sums).astype(jnp.bfloat16)
        mixer_sum = mixer_sum + round_trip(jnp.dot(hidden, down_weight[cols], preferred_element_type=jnp.float32))
    return (middle_f + mixer_sum).astype(jnp.bfloat16)
```

```python
import functools
import math

import jax
import jax.numpy as jnp
from jax import lax
from jax.experimental import pallas as pl
from jax.experimental.pallas import tpu as pltpu
from jax.sharding import PartitionSpec as P

MESH = pl.DeviceIdType.MESH
HEAD_A = 256
HEAD_B = 32
PACK = 640
TILE = 512
SUB = 256
CORES = 2
NY = 4

epsilon = 1e-06


def cut_along(x, dim, devices):
    shape = x.shape
    pieces = x.reshape(*shape[:dim], devices, shape[dim] // devices, *shape[dim + 1 :])
    return jnp.moveaxis(pieces, dim, 0)


def summed_on_arrival(x, axis, dim):
    devices = lax.axis_size(axis)
    pieces = lax.all_to_all(cut_along(x, dim, devices), axis, 0, 0, tiled=True)
    return jnp.sum(pieces.astype(jnp.float32), axis=0)


def turned_gather(arrays, axis, dims):
    turned = [jnp.moveaxis(a, dim, 0) for a, dim in zip(arrays, dims)]
    both = jnp.concatenate([t.reshape(len(t), -1) for t in turned], axis=1)
    result, at, gathered = (lax.all_gather(both, axis, axis=0, tiled=True), 0, [])
    for t, dim in zip(turned, dims):
        section = result[:, at : at + t[0].size].reshape(-1, *t.shape[1:])
        gathered.append(jnp.moveaxis(section, 0, dim))
        at += t[0].size
    return tuple(gathered)


def joined_along(pieces, dim):
    pieces = jnp.moveaxis(pieces, 0, dim)
    shape = pieces.shape
    return pieces.reshape(*shape[:dim], shape[dim] * shape[dim + 1], *shape[dim + 2 :])


def copy_for_each(x, axis):
    copies = jnp.broadcast_to(x, (lax.axis_size(axis), *x.shape))
    return lax.all_to_all(copies, axis, split_axis=0, concat_axis=0, tiled=True)


def gather_directly(x, axis, dim):
    return joined_along(copy_for_each(x, axis), dim)


def gather_kernel(nz, ny, cuts, x_ref, o_ref, send_sem, recv_sem, pair_send, pair_recv, own_sem):
    rows = x_ref.shape[0]
    me = lax.axis_index("sp")
    c = lax.rem(me, CORES)
    y = lax.rem(me // CORES, ny)
    z = me // (CORES * ny)

    def device(zz, yy, cc):
        return (zz * ny + yy) * CORES + cc

    partner = device(z, y, 1 - c)
    around = {
        ("y", 1): device(z, lax.rem(y + 1, ny), c),
        ("y", -1): device(z, lax.rem(y + ny - 1, ny), c),
        ("z", 1): device(lax.rem(z + 1, nz), y, c),
        ("z", -1): device(lax.rem(z + nz - 1, nz), y, c),
    }
    barrier = pltpu.get_barrier_semaphore()
    for other in (partner, *around.values()):
        pl.semaphore_signal(barrier, inc=1, device_id={"sp": other}, device_id_type=MESH)
    pl.semaphore_wait(barrier, 5)

    size = {"y": ny, "z": nz}
    colours = []
    at = 0
    for n, (first, second, way) in enumerate(
        (("y", "z", 1), ("y", "z", -1), ("z", "y", 1), ("z", "y", -1))
    ):
        colours.append((n, first, second, way, at, cuts[n]))
        at += cuts[n]

    def block(ref_rows_of, start, count):
        return o_ref.at[pl.ds(pl.multiple_of(ref_rows_of + start, 8), count)]

    def base_of(zz, yy):
        return device(zz, yy, c) * rows

    own = base_of(z, y)
    own_copy = pltpu.make_async_copy(x_ref, o_ref.at[pl.ds(pl.multiple_of(own, 8), rows)], own_sem)
    own_copy.start()
    pltpu.make_async_remote_copy(
        src_ref=x_ref,
        dst_ref=o_ref.at[pl.ds(pl.multiple_of(own, 8), rows)],
        send_sem=pair_send,
        recv_sem=pair_recv,
        device_id={"sp": partner},
        device_id_type=MESH,
    ).start()

    def send(src, dst, n, index, target):
        pltpu.make_async_remote_copy(
            src_ref=src,
            dst_ref=dst,
            send_sem=send_sem.at[n],
            recv_sem=recv_sem.at[n, index],
            device_id={"sp": target},
            device_id_type=MESH,
        ).start()

    for n, first, second, way, start, count in colours:
        src = x_ref.at[pl.ds(start, count)]
        dst = block(own, start, count)
        send(src, dst, n, 0, around[first, way])
        send(src, dst, n, size[first] - 1, around[second, way])

    def round_of(r, carry):
        for n, first, second, way, start, count in colours:
            na, nb = size[first], size[second]
            early = r < na - 1
            late = r - (na - 1)
            k = jnp.where(early, r + 1, lax.rem(late + na, na))
            m = jnp.where(early, 0, (late + na) // na)
            if first == "y":
                zz = lax.rem(z - way * m + nz, nz)
                yy = lax.rem(y - way * k + ny, ny)
            else:
                zz = lax.rem(z - way * k + nz, nz)
                yy = lax.rem(y - way * m + ny, ny)
            piece = block(base_of(zz, yy), start, count)
            pltpu.make_async_remote_copy(
                src_ref=piece,
                dst_ref=piece,
                send_sem=send_sem.at[n],
                recv_sem=recv_sem.at[n, r],
                device_id={"sp": partner},
                device_id_type=MESH,
            ).wait_recv()

            @pl.when(r < na - 2)
            def _():
                send(piece, piece, n, r + 1, around[first, way])

            @pl.when(early)
            def _():
                send(piece, piece, n, na + r, around[second, way])

            @pl.when(jnp.logical_and(r >= na - 1, r < (na - 1) + (nb - 2) * na))
            def _():
                send(piece, piece, n, r + na, around[second, way])

            pltpu.make_async_remote_copy(
                src_ref=piece,
                dst_ref=piece,
                send_sem=pair_send,
                recv_sem=pair_recv,
                device_id={"sp": partner},
                device_id_type=MESH,
            ).start()
        return carry

    lax.fori_loop(0, nz * ny - 1, round_of, 0)

    def drained(sem, count):
        part = o_ref.at[pl.ds(0, count)]
        pltpu.make_async_copy(part, part, sem).wait()

    own_copy.wait()
    for n, first, second, way, start, count in colours:
        drained(send_sem.at[n], (nz * ny - 1) * count)
    drained(pair_send, nz * ny * rows)
    drained(pair_recv, nz * ny * rows)


def gathered_rows(packed, nz, ny, cuts):
    rows = packed.shape[0]
    return pl.pallas_call(
        functools.partial(gather_kernel, nz, ny, cuts),
        name="gather_rows",
        out_shape=jax.ShapeDtypeStruct((nz * ny * CORES * rows, packed.shape[1]), packed.dtype),
        in_specs=[pl.BlockSpec(memory_space=pltpu.VMEM)],
        out_specs=pl.BlockSpec(memory_space=pl.ANY),
        scratch_shapes=[
            pltpu.SemaphoreType.DMA((4,)),
            pltpu.SemaphoreType.DMA((4, nz * ny - 1)),
            pltpu.SemaphoreType.DMA,
            pltpu.SemaphoreType.DMA,
            pltpu.SemaphoreType.DMA,
        ],
        compiler_params=pltpu.CompilerParams(
            collective_id=0, has_side_effects=True, vmem_limit_bytes=8 * 1024 * 1024
        ),
        cost_estimate=pl.CostEstimate(flops=10**10, bytes_accessed=10**7, transcendentals=0),
    )(packed)


def attention_kernel(
    tiles, tile, anchor_ref, qa_ref, qb_ref, kv_ref, outa_ref, outb_ref, suffix, acca, accb, below
):
    step = pl.program_id(0)
    rows = qa_ref.shape[0]
    anchor = anchor_ref[0]
    start = (tiles - 1 - step) * tile
    nt = (((1,), (1,)), ((), ()))

    @pl.when(step == 0)
    def _():
        suffix[...] = jnp.zeros_like(suffix)
        acca[...] = jnp.zeros_like(acca)
        accb[...] = jnp.zeros_like(accb)
        j = lax.broadcasted_iota(jnp.int32, (SUB, SUB), 0)
        s = lax.broadcasted_iota(jnp.int32, (SUB, SUB), 1)
        below[...] = (j > s).astype(jnp.bfloat16)

    def work(masked):
        for part in reversed(range(tile // SUB)):
            span = pl.ds(part * SUB, SUB)
            if masked:
                key_pos = start + part * SUB + lax.broadcasted_iota(jnp.int32, (rows, SUB), 1)
                query_pos = anchor + lax.broadcasted_iota(jnp.int32, (rows, SUB), 0)
                causal = key_pos < query_pos
            for head, (q_ref, acc, first, width, value, size) in enumerate(
                (
                    (qa_ref, acca, 0, HEAD_A, HEAD_A, HEAD_A),
                    (qb_ref, accb, 2 * HEAD_A, 128, 2 * HEAD_A, HEAD_B),
                )
            ):
                scale = size**-0.5 * math.log2(math.e)
                u = (
                    lax.dot_general(
                        q_ref[...],
                        kv_ref[span, pl.ds(first, width)],
                        nt,
                        preferred_element_type=jnp.float32,
                    )
                    * scale
                )
                soft = jnp.maximum(u, jnp.log2(1.0 + jnp.exp2(jnp.minimum(u, 126.0))))
                if masked:
                    soft = jnp.where(causal, soft, 0.0)
                later = jnp.dot(
                    soft.astype(jnp.bfloat16), below[...], preferred_element_type=jnp.float32
                )
                power = (u - soft) - (later + suffix[head])
                if masked:
                    power = jnp.where(causal, power, -1e30)
                weight = jnp.exp2(power).astype(jnp.bfloat16)
                suffix[head] += jnp.sum(soft, axis=1, keepdims=True)
                acc[...] += jnp.dot(
                    weight,
                    kv_ref[span, pl.ds(value, width)],
                    preferred_element_type=jnp.float32,
                )

    @pl.when(jnp.logical_and(start + tile > anchor, start < anchor + rows))
    def _():
        work(True)

    @pl.when(start + tile <= anchor)
    def _():
        work(False)

    @pl.when(step == tiles - 1)
    def _():
        outa_ref[...] = acca[...].astype(outa_ref.dtype)
        outb_ref[...] = accb[...].astype(outb_ref.dtype)


def attended(anchor, query_a, query_b, kv, tile=TILE):
    rows = query_a.shape[0]
    length = kv.shape[0]
    tiles = length // tile
    return pl.pallas_call(
        functools.partial(attention_kernel, tiles, tile),
        name="stick_attention",
        grid_spec=pltpu.PrefetchScalarGridSpec(
            num_scalar_prefetch=1,
            grid=(tiles,),
            in_specs=[
                pl.BlockSpec((rows, HEAD_A), lambda i, a: (0, 0)),
                pl.BlockSpec((rows, 128), lambda i, a: (0, 0)),
                pl.BlockSpec((tile, PACK), lambda i, a: (tiles - 1 - i, 0)),
            ],
            out_specs=[
                pl.BlockSpec((rows, HEAD_A), lambda i, a: (0, 0)),
                pl.BlockSpec((rows, 128), lambda i, a: (0, 0)),
            ],
            scratch_shapes=[
                pltpu.VMEM((2, rows, 1), jnp.float32),
                pltpu.VMEM((rows, HEAD_A), jnp.float32),
                pltpu.VMEM((rows, 128), jnp.float32),
                pltpu.VMEM((SUB, SUB), jnp.bfloat16),
            ],
        ),
        out_shape=[
            jax.ShapeDtypeStruct((rows, HEAD_A), jnp.bfloat16),
            jax.ShapeDtypeStruct((rows, 128), jnp.bfloat16),
        ],
        compiler_params=pltpu.CompilerParams(
            dimension_semantics=("arbitrary",), vmem_limit_bytes=32 * 1024 * 1024
        ),
        cost_estimate=pl.CostEstimate(
            flops=12 * rows * length * HEAD_A,
            bytes_accessed=length * PACK * 2,
            transcendentals=6 * rows * length,
        ),
    )(anchor, query_a, query_b, kv)


def round_trip(values):
    return lax.optimization_barrier(values.astype(jnp.bfloat16)).astype(jnp.float32)


def row_norm(values, gain_row):
    return (
        values * lax.rsqrt(jnp.mean(values * values, axis=-1, keepdims=True) + epsilon) * gain_row
    )


def body(
    resid,
    query_a,
    key_a,
    value_a,
    query_b,
    key_b,
    value_b,
    out_a,
    out_b,
    attn_gain,
    mlp_gain,
    gate_weight,
    up_weight,
    down_weight,
):
    rows_here = query_a.shape[0]
    chips = lax.axis_size("sp") // CORES
    gate_whole, up_whole, down_whole = turned_gather(
        (gate_weight, up_weight, down_weight), "sp", (0, 0, 1)
    )
    spare = jnp.zeros((rows_here, PACK - 2 * HEAD_A - 2 * HEAD_B), jnp.bfloat16)
    packed = jnp.concatenate([key_a, value_a, key_b, value_b, spare], axis=1)
    kv = gathered_rows(packed, chips // NY, NY, (40, 40, 56, 56))
    anchor = (lax.axis_index("sp") * rows_here).astype(jnp.int32).reshape(1)
    query_b = jnp.pad(query_b, ((0, 0), (0, 128 - HEAD_B)))
    attended_a, wide_b = attended(anchor, query_a, query_b, kv)
    attended_b = wide_b[:, HEAD_B : 2 * HEAD_B]
    term = jnp.dot(attended_a, out_a, preferred_element_type=jnp.float32)
    term = term + jnp.dot(attended_b, out_b, preferred_element_type=jnp.float32)
    projected = summed_on_arrival(round_trip(term).astype(jnp.bfloat16), "tp", 0)
    middle = (resid.astype(jnp.float32) + row_norm(projected, attn_gain)).astype(jnp.bfloat16)
    middle_f = middle.astype(jnp.float32)
    normed_rows = row_norm(middle_f, mlp_gain).astype(jnp.bfloat16)
    channel_input = gather_directly(normed_rows, "tp", 0)
    gate_sums = jnp.dot(channel_input, gate_whole, preferred_element_type=jnp.float32)
    up_sums = jnp.dot(channel_input, up_whole, preferred_element_type=jnp.float32)
    hidden = (jax.nn.silu(gate_sums) * up_sums).astype(jnp.bfloat16)
    mixer_sum = summed_on_arrival(
        round_trip(jnp.dot(hidden, down_whole, preferred_element_type=jnp.float32)).astype(
            jnp.bfloat16
        ),
        "tp",
        0,
    )
    return (middle_f + mixer_sum).astype(jnp.bfloat16)


def solution(mesh):
    return jax.shard_map(
        body,
        mesh=mesh,
        in_specs=(
            P(("sp", "tp"), None),
            P("sp", "tp"),
            P("sp", "tp"),
            P("sp", "tp"),
            P("sp", "tp"),
            P("sp", "tp"),
            P("sp", "tp"),
            P("tp", None),
            P("tp", None),
            P(),
            P(),
            P("sp", "tp"),
            P("sp", "tp"),
            P("tp", "sp"),
        ),
        out_specs=P(("sp", "tp"), None),
        check_vma=False,
    )
```
